32 devices in a mesh: dp: 4 (over y, x), kv: 4 (over z), tp: 2 (over core).
Axes of the slice: x: 2, y: 2, z: 4, core: 2. Of those that a mesh axis runs over, the one named last changes fastest.
Arguments:
- tokens: bfloat16 [4, 1536, 2048], P('dp', 'kv'), may hold values from -21 to 21
- seq_lengths: int32 [4], P('dp'), may hold values from 1 to 1536, 2304 in all
- block_picks: int32 [4, 24, 4, 16], P('dp', 'kv', 'tp'), may hold values from -1 to 17, as said below
- w_query: bfloat16 [2048, 1024], P('kv', 'tp'), may hold values from -0.125 to 0.125
- w_key: bfloat16 [2048, 256], P('kv', 'tp'), may hold values from -0.125 to 0.125
- w_value: bfloat16 [2048, 256], P('kv', 'tp'), may hold values from -0.125 to 0.125
- w_gate: bfloat16 [2048, 32], replicated, may hold values from -0.125 to 0.125
- w_ckey: bfloat16 [4096, 64], replicated, may hold values from -0.09375 to 0.09375
- w_cvalue: bfloat16 [4096, 64], replicated, may hold values from -0.09375 to 0.09375
- w_out: bfloat16 [1024, 2048], P('tp', 'kv'), may hold values from -0.1875 to 0.1875
Outputs:
- attention_out: bfloat16 [4, 1536, 2048], P('dp', ('kv', 'tp'))
The draws below stay inside these ranges and needn't reach their ends.
Inputs may be any that keep to these rules, and one draw needn't show every extreme that they name: `block_picks`: A query block's entries name distinct blocks that all lie in earlier spans of 384 positions, or are -1; the largest such block is named in every draw. For one span and one group, the entries of all its query blocks together name blocks of any one other span at most 2 times; this is reached in every draw.
All inputs are finite; a program needn't handle non-finite values. No bound on the sum of `seq_lengths` on one device may be relied on, other than what follows from the above.
Results may differ from the reference program's by a relative error of at most 0.01.
The reference program's roundings to bfloat16 on the way count: a program that leaves them out, or rounds other values in their place, can miss the bound.
Values may be sent and summed in bfloat16 or wider, within the bound.
No kernel may reach another device: no remote copies, remote signals or barrier semaphores. Data moves between devices by JAX's collectives and lax.ppermute only.
A program may use at most 64 MiB of HBM per device.

```python
import math
import jax
import jax.numpy as jnp
import numpy as np
from jax import lax

D = 2048
HEADS = 16
GROUPS = 4
HEAD = 64
BLK = 64
PICKS = 16
CAP = 2
TOK_DEV = 384
SEQS = 4
SEQ_LEN = 1536
HEAD_SETS = 2


def draw_tokens(key, part):
    grid_shape = (SEQS, SEQ_LEN, D)
    return jnp.clip(jax.random.normal(jax.random.fold_in(key, 20), grid_shape, jnp.float32), -6.0, 6.0).astype(jnp.bfloat16)


def draw_block_picks(key, part):
    span_count = SEQ_LEN // TOK_DEV
    per_span = TOK_DEV // BLK
    slot_total = per_span * PICKS
    grid_shape = (SEQS, span_count, GROUPS, span_count)
    random_order = jax.random.randint(jax.random.fold_in(key, 11), grid_shape, 0, 1 << 20)
    shifts = jax.random.randint(jax.random.fold_in(key, 12), grid_shape, 0, per_span)
    current = jnp.arange(span_count, dtype=jnp.int32)[None, :, None, None]
    candidate = jnp.arange(span_count, dtype=jnp.int32)[None, None, None, :]
    at_end = (current == span_count - 1) & (candidate == span_count - 2)
    shifts = jnp.where(at_end, per_span - 1, shifts)
    ranking = random_order * span_count + candidate
    ranking = jnp.where(candidate == 0, -3, ranking)
    ranking = jnp.where(candidate == current - 1, -4, ranking)
    ranking = jnp.where(candidate == current - span_count // 2, -1, ranking)
    ranking = jnp.where(candidate >= current, (1 << 20) * span_count + candidate, ranking)
    ordered = jnp.argsort(ranking, axis=-1).astype(jnp.int32)
    slots = jnp.arange(slot_total, dtype=jnp.int32)
    places = jnp.minimum(slots // CAP, span_count - 1)
    owners = jnp.take(ordered, places, axis=-1)
    offsets = jnp.take_along_axis(shifts, owners, axis=-1)
    inside = (offsets + slots % CAP) % per_span
    blocks = owners * per_span + inside
    is_valid = (slots // CAP)[None, None, None, :] < current
    picked = jnp.where(is_valid, blocks, -1)
    picked = picked.reshape(SEQS, span_count, GROUPS, per_span, PICKS).transpose(0, 1, 3, 2, 4)
    return picked.reshape(SEQS, span_count * per_span, GROUPS, PICKS).astype(jnp.int32)


def block_levels(own_key, shape, cuts, smallest, largest):
    gain = 1.0
    for dim, blocks in cuts:
        heights = jax.random.uniform(jax.random.fold_in(jax.random.fold_in(own_key, 6), dim), (blocks,), jnp.float32, smallest / len(cuts), largest / len(cuts))
        gain = gain * jnp.repeat(jnp.exp(heights), shape[dim] // blocks).reshape((-1,) + (1,) * (len(shape) - 1 - dim))
    return gain


def profile(number_of, total, limit, lean):
    portions = [(1 << 20) // math.isqrt(rank ** lean) + 1 for rank in range(2, number_of + 1)]
    rest, given = total - limit - (number_of - 1), [1] * (number_of - 1)
    while rest > 0:
        free = [i for i in range(number_of - 1) if given[i] < limit]
        whole, remaining = sum([portions[i] for i in free]), rest
        for i in free:
            extra = min(limit - given[i], max(1, remaining * portions[i] // whole), rest)
            given[i] = given[i] + extra
            rest = rest - extra
    return np.array([limit] + given)


def ragged(key, amount, total, reach, skew):
    if amount == 2:
        one = jax.random.randint(key, (), max(1, total - reach), min(reach, total - 1) + 1)
        return jnp.stack([one, total - one])
    tallies = jnp.asarray(profile(amount, total, reach, skew), jnp.int32)
    pairs = (amount - 1) // 2
    giver, receiver = tallies[1:1 + 2 * pairs:2], tallies[2:2 + 2 * pairs:2]
    room = jnp.minimum(giver - 1, reach - receiver)
    shifted = jax.random.randint(jax.random.fold_in(key, 1), (pairs,), 0, 1 << 20) % (room + 1)
    tallies = tallies.at[1:1 + 2 * pairs:2].set(giver - shifted).at[2:2 + 2 * pairs:2].set(receiver + shifted)
    return tallies[jax.random.permutation(jax.random.fold_in(key, 2), amount)]


def normal_values(stream_key, dims, scale, most, shards=(), held_as=jnp.bfloat16):
    drawn = scale * jax.random.normal(stream_key, dims, jnp.float32)
    if shards:
        drawn = drawn * block_levels(stream_key, dims, shards, -0.22, 0.18)
    return jnp.clip(drawn, -most, most).astype(held_as)


def setup_inputs(seed: int = 0) -> dict:
    key_of = jax.random.split(jax.random.key(seed), 11)
    tokens = draw_tokens(jax.random.fold_in(key_of[10], 71), 0)
    seq_lengths = ragged(key_of[1], SEQS, 3 * SEQS * SEQ_LEN // 8, SEQ_LEN, 2).astype(jnp.int32)
    block_picks = draw_block_picks(jax.random.fold_in(key_of[10], 71), 0)
    w_query = normal_values(key_of[3], (D, HEADS * HEAD), D ** -0.5, 0.125, ((0, 4), (1, 2)))
    w_key = normal_values(key_of[4], (D, GROUPS * HEAD), D ** -0.5, 0.125, ((0, 4), (1, 2)))
    w_value = normal_values(key_of[5], (D, GROUPS * HEAD), D ** -0.5, 0.125, ((0, 4), (1, 2)))
    w_gate = normal_values(key_of[6], (D, 2 * HEADS), D ** -0.5, 0.125)
    w_ckey = normal_values(key_of[7], (BLK * HEAD, HEAD), (BLK * HEAD) ** -0.5, 0.09375)
    w_cvalue = normal_values(key_of[8], (BLK * HEAD, HEAD), (BLK * HEAD) ** -0.5, 0.09375)
    w_out = normal_values(key_of[9], (HEADS * HEAD, D), (HEADS * HEAD) ** -0.5, 0.1875, ((0, 2), (1, 4)))
    return dict(tokens=tokens, seq_lengths=seq_lengths, block_picks=block_picks, w_query=w_query, w_key=w_key, w_value=w_value, w_gate=w_gate, w_ckey=w_ckey, w_cvalue=w_cvalue, w_out=w_out)


masked_low = -1e30


def reference(tokens, seq_lengths, block_picks, w_query, w_key, w_value, w_gate, w_ckey, w_cvalue, w_out):
    per_group = HEADS // GROUPS
    block_total = SEQ_LEN // BLK
    inv_scale = HEAD ** -0.5
    set_width = HEADS * HEAD // HEAD_SETS
    causal = jnp.arange(BLK)[None, :] <= jnp.arange(BLK)[:, None]
    block_ends = jnp.arange(block_total, dtype=jnp.int32) * BLK + (BLK - 1)
    group_ids = jnp.arange(GROUPS, dtype=jnp.int32)

    def sequence(inputs):
        token_rows, length, picked = inputs
        queries = jnp.dot(token_rows, w_query, preferred_element_type=jnp.float32).astype(jnp.bfloat16)
        queries = lax.optimization_barrier(queries).reshape(block_total, BLK, GROUPS, per_group, HEAD)
        keys_all = jnp.dot(token_rows, w_key, preferred_element_type=jnp.float32).astype(jnp.bfloat16)
        keys_all = keys_all.reshape(block_total, BLK, GROUPS, HEAD).transpose(0, 2, 1, 3)
        values_all = jnp.dot(token_rows, w_value, preferred_element_type=jnp.float32).astype(jnp.bfloat16)
        values_all = values_all.reshape(block_total, BLK, GROUPS, HEAD).transpose(0, 2, 1, 3)
        keys_all = lax.optimization_barrier(keys_all)
        values_all = lax.optimization_barrier(values_all)
        gate_all = jax.nn.sigmoid(jnp.dot(token_rows, w_gate, preferred_element_type=jnp.float32))
        gate_all = gate_all.reshape(block_total, BLK, 2, GROUPS, per_group)
        ckeys = jnp.dot(keys_all.reshape(block_total * GROUPS, BLK * HEAD), w_ckey,
                        preferred_element_type=jnp.float32).astype(jnp.bfloat16)
        cvalues = jnp.dot(values_all.reshape(block_total * GROUPS, BLK * HEAD), w_cvalue,
                          preferred_element_type=jnp.float32).astype(jnp.bfloat16)
        ckeys = lax.optimization_barrier(ckeys).reshape(block_total, GROUPS, HEAD).astype(jnp.float32)
        cvalues = lax.optimization_barrier(cvalues).reshape(block_total, GROUPS, HEAD).astype(jnp.float32)

        def attend(block_inputs):
            qblock, gblock, picked_row, block_index = block_inputs
            qfloat = qblock.astype(jnp.float32)
            query_spots = block_index * BLK + jnp.arange(BLK, dtype=jnp.int32)
            comp_score = jnp.einsum('tgpd,cgd->gtpc', qfloat, ckeys) * inv_scale
            visible = (block_ends[None, :] <= query_spots[:, None])[None, :, None, :]
            comp_score = jnp.where(visible, comp_score, masked_low)
            comp_top = jnp.max(comp_score, axis=-1, keepdims=True)
            comp_weight = jnp.where(visible, jnp.exp(comp_score - comp_top), 0.0)
            comp_sum = jnp.maximum(jnp.sum(comp_weight, axis=-1, keepdims=True), 1.0)
            comp_prob = lax.optimization_barrier((comp_weight / comp_sum).astype(jnp.bfloat16))
            comp_out = jnp.einsum('gtpc,cgd->tgpd', comp_prob.astype(jnp.float32), cvalues)
            own_keys = keys_all[block_index].astype(jnp.float32)
            own_values = values_all[block_index].astype(jnp.float32)
            usable = picked_row >= 0
            safe_picks = jnp.where(usable, picked_row, 0)
            far_keys = keys_all[safe_picks, group_ids[:, None]].reshape(GROUPS, PICKS * BLK, HEAD).astype(jnp.float32)
            far_values = values_all[safe_picks, group_ids[:, None]].reshape(GROUPS, PICKS * BLK, HEAD).astype(jnp.float32)
            own_score = jnp.einsum('tgpd,gsd->gtps', qfloat, own_keys) * inv_scale
            own_mask = causal[None, :, None, :]
            own_score = jnp.where(own_mask, own_score, masked_low)
            far_score = jnp.einsum('tgpd,gkd->gtpk', qfloat, far_keys) * inv_scale
            far_mask = jnp.repeat(usable, BLK, axis=-1)[:, None, None, :]
            far_score = jnp.where(far_mask, far_score, masked_low)
            score_top = jnp.maximum(jnp.max(own_score, axis=-1, keepdims=True),
                                    jnp.max(far_score, axis=-1, keepdims=True))
            own_weight = jnp.where(own_mask, jnp.exp(own_score - score_top), 0.0)
            far_weight = jnp.where(far_mask, jnp.exp(far_score - score_top), 0.0)
            normalizer = jnp.sum(own_weight, axis=-1, keepdims=True) + jnp.sum(far_weight, axis=-1, keepdims=True)
            own_prob = lax.optimization_barrier((own_weight / normalizer).astype(jnp.bfloat16))
            far_prob = lax.optimization_barrier((far_weight / normalizer).astype(jnp.bfloat16))
            chosen_out = (jnp.einsum('gtps,gsd->tgpd', own_prob.astype(jnp.float32), own_values)
                          + jnp.einsum('gtpk,gkd->tgpd', far_prob.astype(jnp.float32), far_values))
            mixed_out = gblock[:, 0, :, :, None] * comp_out + gblock[:, 1, :, :, None] * chosen_out
            return mixed_out.astype(jnp.bfloat16)

        attended = lax.map(attend, (queries, gate_all, picked, jnp.arange(block_total, dtype=jnp.int32)))
        attended = attended.reshape(SEQ_LEN, HEAD_SETS, set_width)
        weight_sets = w_out.reshape(HEAD_SETS, set_width, D)
        summed = jnp.zeros((SEQ_LEN, D), jnp.float32)
        for set_index in range(HEAD_SETS):
            partial_out = jnp.dot(attended[:, set_index], weight_sets[set_index],
                                  preferred_element_type=jnp.float32).astype(jnp.bfloat16)
            summed = summed + lax.optimization_barrier(partial_out).astype(jnp.float32)
        live_rows = jnp.arange(SEQ_LEN, dtype=jnp.int32) < length
        return jnp.where(live_rows[:, None], summed, 0.0).astype(jnp.bfloat16)

    return lax.map(sequence, (tokens, seq_lengths, block_picks))
```

```python
import functools

import jax
import jax.numpy as jnp
from jax import lax
from jax.experimental import pallas as pl
from jax.experimental.pallas import tpu as pltpu
from jax.sharding import PartitionSpec as P

HEADS = 16
HEAD = 64
BLK = 64
PICKS = 16
LANES = 128

masked_low = -1e30


def nt_dot(a, b):
    return lax.dot_general(a, b, (((1,), (1,)), ((), ())), preferred_element_type=jnp.float32)


def group_slabs(slab, odd, low_lanes, high_lanes):
    rolled = jnp.concatenate([slab[:, HEAD:], slab[:, :HEAD]], axis=1)
    low, high = (rolled, slab) if odd else (slab, rolled)
    return jnp.concatenate([low * low_lanes, high * high_lanes], axis=0)


def attend_kernel(
    shape, start_ref, picks_ref, q_ref, gate_ref, pairs_ref, comp_ref, out_ref, spill_ref, list_ref
):
    blocks, groups, per_group, span_rows = shape
    pairs = per_group // 2
    rows = pairs * BLK
    kv_width = groups * HEAD
    comp_count = comp_ref.shape[0]
    inv_scale = HEAD ** (-0.5)
    span = start_ref[0]
    lane_row = lax.broadcasted_iota(jnp.int32, (1, LANES), 1)
    low_lanes = jnp.where(lane_row < HEAD, 1.0, 0.0).astype(jnp.bfloat16)
    high_lanes = jnp.where(lane_row < HEAD, 0.0, 1.0).astype(jnp.bfloat16)
    lane = lax.broadcasted_iota(jnp.int32, (rows, LANES), 1)
    spot = lax.broadcasted_iota(jnp.int32, (rows, LANES), 0) % BLK
    low_half = lane < HEAD
    own_seen = low_half & (lane <= spot)
    high_half = jnp.logical_not(low_half)
    comp_lane = lax.broadcasted_iota(jnp.int32, (rows, comp_count), 1)
    comp_spot = lax.broadcasted_iota(jnp.int32, (rows, comp_count), 0) % BLK

    def block_rows(block):
        at = block // blocks
        row = pl.multiple_of((block - at * blocks) * BLK, BLK)
        return at, pl.ds(row, BLK)

    def two_heads(s, n):
        return s[:, :n], s[:, n:]

    def top(s, mask):
        s = jnp.where(mask, s, masked_low)
        return s, jnp.max(s, axis=1, keepdims=True)

    def key_values(block_a, block_b, g):
        column = (g // 2) * LANES
        parts = []
        for base in (column, kv_width + column):
            a_span, a_rows = block_rows(block_a)
            b_span, b_rows = block_rows(block_b)
            slab = jnp.concatenate(
                [
                    pairs_ref[a_span, a_rows, base : base + LANES],
                    pairs_ref[b_span, b_rows, base : base + LANES],
                ],
                axis=0,
            )
            parts.append(group_slabs(slab, g % 2, low_lanes, high_lanes))
        return parts

    comp_parts = []
    for g in range(groups):
        column = (g // 2) * LANES
        comp_parts.append(
            [
                group_slabs(comp_ref[:, base : base + LANES], g % 2, low_lanes, high_lanes)
                for base in (column, kv_width + column)
            ]
        )

    def one_block(b, _):
        here = pl.ds(pl.multiple_of(b * BLK, BLK), BLK)
        gates = gate_ref[here, :]
        for g in range(groups):
            count = jnp.int32(0)
            for k in range(PICKS):
                pick = picks_ref[b, g * PICKS + k]
                list_ref[count] = pick
                count = count + (pick >= 0).astype(jnp.int32)
            first = jnp.maximum(list_ref[0], 0)
            queries = jnp.concatenate(
                [
                    q_ref[here, (g * pairs + p) * LANES : (g * pairs + p + 1) * LANES]
                    for p in range(pairs)
                ],
                axis=0,
            )
            ckeys, cvalues = comp_parts[g]
            comp_seen = (comp_lane + 1) * BLK - 1 <= (span * blocks + b) * BLK + comp_spot
            comp_probs = []
            for s in two_heads(nt_dot(queries, ckeys) * inv_scale, comp_count):
                s, m = top(s, comp_seen)
                w = jnp.where(comp_seen, jnp.exp(s - m), 0.0)
                total = jnp.maximum(jnp.sum(w, axis=1, keepdims=True), 1.0)
                comp_probs.append((w * (1.0 / total)).astype(jnp.bfloat16))
            comp_out = jnp.dot(
                jnp.concatenate(comp_probs, axis=1), cvalues, preferred_element_type=jnp.float32
            )
            keys, values = key_values(span * blocks + b, first, g)
            seen = own_seen | (high_half & (jnp.full((rows, LANES), count) > 0))
            (s0, m0), (s1, m1) = [
                top(s, seen) for s in two_heads(nt_dot(queries, keys) * inv_scale, LANES)
            ]
            steps = count // 2

            def far_blocks(i):
                second_there = 2 * i + 2 < count
                block_a = list_ref[2 * i + 1]
                block_b = jnp.where(second_there, list_ref[2 * i + 2], block_a)
                return block_a, block_b, second_there

            def scan(i, tops):
                block_a, block_b, second_there = far_blocks(i)
                far_keys, _ = key_values(block_a, block_b, g)
                limit = jnp.where(second_there, LANES, HEAD)
                far_seen = lane < jnp.full((rows, LANES), limit)
                s = two_heads(nt_dot(queries, far_keys) * inv_scale, LANES)
                (a, ma), (c, mc) = [top(x, far_seen) for x in s]
                spill_ref[i, :, :LANES] = a
                spill_ref[i, :, LANES:] = c
                return jnp.maximum(tops[0], ma), jnp.maximum(tops[1], mc)

            m0, m1 = lax.fori_loop(0, steps, scan, (m0, m1))
            w0, w1 = jnp.exp(s0 - m0), jnp.exp(s1 - m1)
            l0 = jnp.sum(w0, axis=1, keepdims=True)
            l1 = jnp.sum(w1, axis=1, keepdims=True)

            def add_up(i, sums):
                a = jnp.exp(spill_ref[i, :, :LANES] - m0)
                c = jnp.exp(spill_ref[i, :, LANES:] - m1)
                spill_ref[i, :, :LANES] = a
                spill_ref[i, :, LANES:] = c
                return (
                    sums[0] + jnp.sum(a, axis=1, keepdims=True),
                    sums[1] + jnp.sum(c, axis=1, keepdims=True),
                )

            l0, l1 = lax.fori_loop(0, steps, add_up, (l0, l1))
            r0, r1 = 1.0 / l0, 1.0 / l1

            def weigh(a, c, far_values):
                probs = jnp.concatenate(
                    [(a * r0).astype(jnp.bfloat16), (c * r1).astype(jnp.bfloat16)], axis=1
                )
                return jnp.dot(probs, far_values, preferred_element_type=jnp.float32)

            def gather(i, total):
                block_a, block_b, _ = far_blocks(i)
                _, far_values = key_values(block_a, block_b, g)
                return total + weigh(spill_ref[i, :, :LANES], spill_ref[i, :, LANES:], far_values)

            chosen_out = lax.fori_loop(0, steps, gather, weigh(w0, w1, values))
            for p in range(pairs):
                h = g * per_group + 2 * p
                part = slice(p * BLK, (p + 1) * BLK)
                low = low_half[part]
                mix = []
                for branch in range(2):
                    at = branch * groups * per_group + h
                    mix.append(jnp.where(low, gates[:, at : at + 1], gates[:, at + 1 : at + 2]))
                mixed = mix[0] * comp_out[part] + mix[1] * chosen_out[part]
                column = (g * pairs + p) * LANES
                out_ref[here, column : column + LANES] = mixed.astype(jnp.bfloat16)
        return 0

    lax.fori_loop(0, blocks, one_block, 0)


def attend(shape, span, picks, queries, gates, pairs, comp):
    blocks, groups, per_group, _ = shape
    rows = per_group // 2 * BLK
    smem = pl.BlockSpec(memory_space=pltpu.SMEM)
    vmem = pl.BlockSpec(memory_space=pltpu.VMEM)
    return pl.pallas_call(
        functools.partial(attend_kernel, shape),
        out_shape=jax.ShapeDtypeStruct(queries.shape, jnp.bfloat16),
        in_specs=[smem, smem, vmem, vmem, vmem, vmem],
        out_specs=vmem,
        scratch_shapes=[
            pltpu.VMEM((PICKS // 2, rows, 2 * LANES), jnp.float32),
            pltpu.SMEM((PICKS + 2,), jnp.int32),
        ],
        cost_estimate=pl.CostEstimate(
            flops=int(1e10), bytes_accessed=int(4e6), transcendentals=int(1e6)
        ),
    )(span, picks, queries, gates, pairs, comp)


def body(
    tokens, seq_lengths, block_picks, w_query, w_key, w_value, w_gate, w_ckey, w_cvalue, w_out
):
    token_rows = tokens[0]
    tok_count = token_rows.shape[0]
    width = token_rows.shape[1]
    spans = lax.axis_size("kv")
    copies = lax.axis_size("dp")
    shard_index = lax.axis_index("kv")
    head_index = lax.axis_index("tp")
    group_count = w_key.shape[1] // HEAD
    head_count = w_query.shape[1] // HEAD
    per_group = head_count // group_count
    block_count = tok_count // BLK

    def share(w):
        part = w.shape[0] // copies
        return lax.dynamic_slice_in_dim(w, lax.axis_index("dp") * part, part, 0)

    def gather_rows(w):
        return lax.all_gather(share(w), ("kv", "dp"), axis=0, tiled=True)

    kv_weight = gather_rows(jnp.concatenate([w_key, w_value], axis=1))
    query_weight = gather_rows(w_query)

    kv = jnp.dot(token_rows, kv_weight, preferred_element_type=jnp.float32).astype(jnp.bfloat16)
    split = kv.reshape(block_count, BLK, 2, group_count, HEAD)

    def compress(which, w):
        flat = split[:, :, which].transpose(0, 2, 1, 3).reshape(-1, BLK * HEAD)
        out = jnp.dot(flat, w, preferred_element_type=jnp.float32).astype(jnp.bfloat16)
        return out.reshape(block_count, group_count * HEAD)

    comp = jnp.concatenate([compress(0, w_ckey), compress(1, w_cvalue)], axis=1)
    pad = -block_count % 16
    packed = jnp.concatenate([kv, jnp.pad(comp, ((0, pad), (0, 0)))], axis=0)
    every = lax.all_gather(packed, "kv", axis=0)
    comp_all = every[:, tok_count : tok_count + block_count].reshape(spans * block_count, -1)
    comp_all = jnp.pad(comp_all, ((0, -comp_all.shape[0] % LANES), (0, 0)))

    queries = jnp.dot(token_rows, query_weight, preferred_element_type=jnp.float32)
    queries = queries.astype(jnp.bfloat16)
    gate_all = jax.nn.sigmoid(jnp.dot(token_rows, w_gate, preferred_element_type=jnp.float32))
    gates = lax.dynamic_slice_in_dim(
        gate_all.reshape(tok_count, 2, HEADS), head_index * head_count, head_count, 2
    ).reshape(tok_count, 2 * head_count)

    shape = (block_count, group_count, per_group, tok_count)
    attended = attend(
        shape,
        jnp.full((1,), shard_index, jnp.int32),
        block_picks[0].reshape(block_count, group_count * PICKS),
        queries,
        gates,
        every,
        comp_all,
    )

    out_parts = lax.all_gather(share(w_out), ("kv", "dp"), axis=0)
    out_parts = out_parts.reshape(spans, w_out.shape[0], w_out.shape[1])
    sides = lax.axis_size("tp")
    half_rows = tok_count // sides

    def project(side):
        rows = lax.dynamic_slice_in_dim(attended, side * half_rows, half_rows, 0)
        return [
            jnp.dot(rows, out_parts[i], preferred_element_type=jnp.float32).astype(jnp.bfloat16)
            for i in range(spans)
        ]

    swap = [(i, 1 - i) for i in range(sides)]
    theirs = jnp.concatenate(project(1 - head_index), axis=1)
    came = lax.ppermute(theirs, "tp", swap)
    mine = jnp.concatenate(project(head_index), axis=1)
    summed = mine.astype(jnp.float32) + came.astype(jnp.float32)
    out_positions = (
        shard_index * tok_count + head_index * half_rows + jnp.arange(half_rows, dtype=jnp.int32)
    )
    live_rows = out_positions < seq_lengths[0]
    return jnp.where(live_rows[:, None], summed, 0.0).astype(jnp.bfloat16)[None]


def solution(mesh):
    return jax.shard_map(
        body,
        mesh=mesh,
        in_specs=(
            P("dp", "kv", None),
            P("dp"),
            P("dp", "kv", "tp", None),
            P("kv", "tp"),
            P("kv", "tp"),
            P("kv", "tp"),
            P(),
            P(),
            P(),
            P("tp", "kv"),
        ),
        out_specs=P("dp", ("kv", "tp"), None),
        check_vma=False,
    )
```

```python
import functools

import jax
import jax.numpy as jnp
from jax import lax
from jax.experimental import pallas as pl
from jax.experimental.pallas import tpu as pltpu
from jax.sharding import PartitionSpec as P

HEADS = 16
HEAD = 64
BLK = 64
PICKS = 16
LANES = 128

masked_low = -1e30


def nt_dot(a, b):
    return lax.dot_general(a, b, (((1,), (1,)), ((), ())), preferred_element_type=jnp.float32)


def group_slabs(slab, odd, low_lanes, high_lanes):
    rolled = jnp.concatenate([slab[:, HEAD:], slab[:, :HEAD]], axis=1)
    low, high = (rolled, slab) if odd else (slab, rolled)
    return jnp.concatenate([low * low_lanes, high * high_lanes], axis=0)


def attend_kernel(
    shape, start_ref, picks_ref, q_ref, gate_ref, pairs_ref, comp_ref, out_ref, spill_ref, list_ref
):
    blocks, groups, per_group, few = shape
    pairs = per_group // 2
    rows = pairs * BLK
    kv_width = groups * HEAD
    comp_count = comp_ref.shape[0]
    inv_scale = HEAD ** (-0.5)
    span = start_ref[0]
    lane_row = lax.broadcasted_iota(jnp.int32, (1, LANES), 1)
    low_lanes = jnp.where(lane_row < HEAD, 1.0, 0.0).astype(jnp.bfloat16)
    high_lanes = jnp.where(lane_row < HEAD, 0.0, 1.0).astype(jnp.bfloat16)
    lane = lax.broadcasted_iota(jnp.int32, (rows, LANES), 1)
    spot = lax.broadcasted_iota(jnp.int32, (rows, LANES), 0) % BLK
    low_half = lane < HEAD
    own_seen = low_half & (lane <= spot)
    high_half = jnp.logical_not(low_half)
    comp_lane = lax.broadcasted_iota(jnp.int32, (rows, comp_count), 1)
    comp_spot = lax.broadcasted_iota(jnp.int32, (rows, comp_count), 0) % BLK

    def block_rows(block):
        at = block // blocks
        row = pl.multiple_of((block - at * blocks) * BLK, BLK)
        return span - at if few else at, pl.ds(row, BLK)

    def two_heads(s, n):
        return s[:, :n], s[:, n:]

    def top(s, mask):
        s = jnp.where(mask, s, masked_low)
        return s, jnp.max(s, axis=1, keepdims=True)

    def key_values(block_a, block_b, g):
        column = (g // 2) * LANES
        parts = []
        for base in (column, kv_width + column):
            a_span, a_rows = block_rows(block_a)
            b_span, b_rows = block_rows(block_b)
            slab = jnp.concatenate(
                [
                    pairs_ref[a_span, a_rows, base : base + LANES],
                    pairs_ref[b_span, b_rows, base : base + LANES],
                ],
                axis=0,
            )
            parts.append(group_slabs(slab, g % 2, low_lanes, high_lanes))
        return parts

    comp_parts = []
    for g in range(groups):
        column = (g // 2) * LANES
        comp_parts.append(
            [
                group_slabs(comp_ref[:, base : base + LANES], g % 2, low_lanes, high_lanes)
                for base in (column, kv_width + column)
            ]
        )

    def one_block(b, _):
        here = pl.ds(pl.multiple_of(b * BLK, BLK), BLK)
        gates = gate_ref[here, :]
        for g in range(groups):
            count = jnp.int32(0)
            for k in range(PICKS):
                pick = picks_ref[b, g * PICKS + k]
                list_ref[count] = pick
                count = count + (pick >= 0).astype(jnp.int32)
            first = jnp.maximum(list_ref[0], 0)
            queries = jnp.concatenate(
                [
                    q_ref[here, (g * pairs + p) * LANES : (g * pairs + p + 1) * LANES]
                    for p in range(pairs)
                ],
                axis=0,
            )
            ckeys, cvalues = comp_parts[g]
            comp_seen = (comp_lane + 1) * BLK - 1 <= (span * blocks + b) * BLK + comp_spot
            comp_probs = []
            for s in two_heads(nt_dot(queries, ckeys) * inv_scale, comp_count):
                s, m = top(s, comp_seen)
                w = jnp.where(comp_seen, jnp.exp(s - m), 0.0)
                total = jnp.maximum(jnp.sum(w, axis=1, keepdims=True), 1.0)
                comp_probs.append((w * (1.0 / total)).astype(jnp.bfloat16))
            comp_out = jnp.dot(
                jnp.concatenate(comp_probs, axis=1), cvalues, preferred_element_type=jnp.float32
            )
            keys, values = key_values(span * blocks + b, first, g)
            seen = own_seen | (high_half & (jnp.full((rows, LANES), count) > 0))
            (s0, m0), (s1, m1) = [
                top(s, seen) for s in two_heads(nt_dot(queries, keys) * inv_scale, LANES)
            ]
            steps = count // 2

            def far_blocks(i):
                second_there = 2 * i + 2 < count
                block_a = list_ref[2 * i + 1]
                block_b = jnp.where(second_there, list_ref[2 * i + 2], block_a)
                return block_a, block_b, second_there

            def scan(i, tops):
                block_a, block_b, second_there = far_blocks(i)
                far_keys, _ = key_values(block_a, block_b, g)
                limit = jnp.where(second_there, LANES, HEAD)
                far_seen = lane < jnp.full((rows, LANES), limit)
                s = two_heads(nt_dot(queries, far_keys) * inv_scale, LANES)
                (a, ma), (c, mc) = [top(x, far_seen) for x in s]
                spill_ref[i, :, :LANES] = a
                spill_ref[i, :, LANES:] = c
                return jnp.maximum(tops[0], ma), jnp.maximum(tops[1], mc)

            m0, m1 = lax.fori_loop(0, steps, scan, (m0, m1))
            w0, w1 = jnp.exp(s0 - m0), jnp.exp(s1 - m1)
            l0 = jnp.sum(w0, axis=1, keepdims=True)
            l1 = jnp.sum(w1, axis=1, keepdims=True)

            def add_up(i, sums):
                a = jnp.exp(spill_ref[i, :, :LANES] - m0)
                c = jnp.exp(spill_ref[i, :, LANES:] - m1)
                spill_ref[i, :, :LANES] = a
                spill_ref[i, :, LANES:] = c
                return (
                    sums[0] + jnp.sum(a, axis=1, keepdims=True),
                    sums[1] + jnp.sum(c, axis=1, keepdims=True),
                )

            l0, l1 = lax.fori_loop(0, steps, add_up, (l0, l1))
            r0, r1 = 1.0 / l0, 1.0 / l1

            def weigh(a, c, far_values):
                probs = jnp.concatenate(
                    [(a * r0).astype(jnp.bfloat16), (c * r1).astype(jnp.bfloat16)], axis=1
                )
                return jnp.dot(probs, far_values, preferred_element_type=jnp.float32)

            def gather(i, total):
                block_a, block_b, _ = far_blocks(i)
                _, far_values = key_values(block_a, block_b, g)
                return total + weigh(spill_ref[i, :, :LANES], spill_ref[i, :, LANES:], far_values)

            chosen_out = lax.fori_loop(0, steps, gather, weigh(w0, w1, values))
            for p in range(pairs):
                h = g * per_group + 2 * p
                part = slice(p * BLK, (p + 1) * BLK)
                low = low_half[part]
                mix = []
                for branch in range(2):
                    at = branch * groups * per_group + h
                    mix.append(jnp.where(low, gates[:, at : at + 1], gates[:, at + 1 : at + 2]))
                mixed = mix[0] * comp_out[part] + mix[1] * chosen_out[part]
                column = (g * pairs + p) * LANES
                out_ref[here, column : column + LANES] = mixed.astype(jnp.bfloat16)
        return 0

    lax.fori_loop(0, blocks, one_block, 0)


def attend(shape, span, picks, queries, gates, pairs, comp):
    blocks, groups, per_group, _ = shape
    rows = per_group // 2 * BLK
    smem = pl.BlockSpec(memory_space=pltpu.SMEM)
    vmem = pl.BlockSpec(memory_space=pltpu.VMEM)
    return pl.pallas_call(
        functools.partial(attend_kernel, shape),
        out_shape=jax.ShapeDtypeStruct(queries.shape, jnp.bfloat16),
        in_specs=[smem, smem, vmem, vmem, vmem, vmem],
        out_specs=vmem,
        scratch_shapes=[
            pltpu.VMEM((PICKS // 2, rows, 2 * LANES), jnp.float32),
            pltpu.SMEM((PICKS + 2,), jnp.int32),
        ],
        cost_estimate=pl.CostEstimate(
            flops=int(1e10), bytes_accessed=int(4e6), transcendentals=int(1e6)
        ),
    )(span, picks, queries, gates, pairs, comp)


def shard_pieces(w, axis, spans, copies):
    part = w.shape[axis] // copies
    mine = lax.dynamic_slice_in_dim(w, lax.axis_index("dp") * part, part, axis)
    pieces = []
    for s in range(1, spans):
        came = lax.ppermute(mine, "kv", [(i, (i + s) % spans) for i in range(spans)])
        pieces.append(came)
        for m in range(1, copies):
            pieces.append(lax.ppermute(came, "dp", [(i, i ^ m) for i in range(copies)]))
    return pieces


def piece_places(spans, copies, me, copy):
    return [
        (lax.rem(me - s + spans, spans), copy ^ m) for s in range(1, spans) for m in range(copies)
    ]


def project_kernel(spans, copies, at_ref, x_ref, own_ref, *refs):
    *pieces, out_ref = refs
    rows = own_ref.shape[0]
    part = rows // copies
    me, copy = at_ref[0], at_ref[1]
    total = jnp.dot(
        x_ref[:, pl.ds(pl.multiple_of(me * rows, LANES), rows)],
        own_ref[...],
        preferred_element_type=jnp.float32,
    )
    for piece, (span, owner) in zip(pieces, piece_places(spans, copies, me, copy)):
        start = pl.multiple_of(span * rows + owner * part, LANES)
        total = total + jnp.dot(
            x_ref[:, pl.ds(start, part)], piece[...], preferred_element_type=jnp.float32
        )
    out_ref[...] = total.astype(out_ref.dtype)


def out_kernel(spans, copies, at_ref, x_ref, own_ref, *refs):
    *pieces, out_ref = refs
    width = own_ref.shape[1]
    part = width // copies
    me, copy, side = at_ref[0], at_ref[1], at_ref[2]
    count = out_ref.shape[0]
    x = x_ref[pl.ds(pl.multiple_of(side * count, 16), count), :]
    start = pl.multiple_of(me * width, LANES)
    out_ref[:, pl.ds(start, width)] = jnp.dot(
        x, own_ref[...], preferred_element_type=jnp.float32
    ).astype(out_ref.dtype)
    for piece, (span, owner) in zip(pieces, piece_places(spans, copies, me, copy)):
        start = pl.multiple_of(span * width + owner * part, LANES)
        out_ref[:, pl.ds(start, part)] = jnp.dot(
            x, piece[...], preferred_element_type=jnp.float32
        ).astype(out_ref.dtype)


def piece_product(kernel, spans, copies, at, x, own, pieces, out_dims):
    vmem = pl.BlockSpec(memory_space=pltpu.VMEM)
    return pl.pallas_call(
        functools.partial(kernel, spans, copies),
        out_shape=jax.ShapeDtypeStruct(out_dims, jnp.bfloat16),
        in_specs=[pl.BlockSpec(memory_space=pltpu.SMEM)] + [vmem] * (2 + len(pieces)),
        out_specs=vmem,
        cost_estimate=pl.CostEstimate(
            flops=2 * out_dims[0] * out_dims[1] * x.shape[1],
            bytes_accessed=int(4e6),
            transcendentals=0,
        ),
    )(at, x, own, *pieces)


def body(
    tokens, seq_lengths, block_picks, w_query, w_key, w_value, w_gate, w_ckey, w_cvalue, w_out
):
    token_rows = tokens[0]
    tok_count = token_rows.shape[0]
    width = token_rows.shape[1]
    spans = lax.axis_size("kv")
    copies = lax.axis_size("dp")
    sides = lax.axis_size("tp")
    shard_index = lax.axis_index("kv")
    head_index = lax.axis_index("tp")
    copy_index = lax.axis_index("dp")
    group_count = w_key.shape[1] // HEAD
    head_count = w_query.shape[1] // HEAD
    per_group = head_count // group_count
    block_count = tok_count // BLK
    half_rows = tok_count // sides
    w_both = jnp.concatenate([w_key, w_value], axis=1)
    few = spans <= 8 and w_both.shape[0] % (copies * LANES) == 0 and copies & (copies - 1) == 0

    def place(side):
        return jnp.stack([shard_index, copy_index, side]).astype(jnp.int32)

    def share(w):
        part = w.shape[0] // copies
        return lax.dynamic_slice_in_dim(w, copy_index * part, part, 0)

    def project(w, pieces):
        if few:
            dims = (tok_count, w.shape[1])
            at = place(head_index)
            return piece_product(project_kernel, spans, copies, at, token_rows, w, pieces, dims)
        whole = lax.all_gather(share(w), ("kv", "dp"), axis=0, tiled=True)
        out = jnp.dot(token_rows, whole, preferred_element_type=jnp.float32)
        return out.astype(jnp.bfloat16)

    kv_pieces = query_pieces = out_pieces = None
    if few:
        kv_pieces = shard_pieces(w_both, 0, spans, copies)
        query_pieces = shard_pieces(w_query, 0, spans, copies)
        out_pieces = shard_pieces(w_out, 1, spans, copies)

    gate_all = jax.nn.sigmoid(jnp.dot(token_rows, w_gate, preferred_element_type=jnp.float32))
    gates = lax.dynamic_slice_in_dim(
        gate_all.reshape(tok_count, 2, HEADS), head_index * head_count, head_count, 2
    ).reshape(tok_count, 2 * head_count)

    kv = project(w_both, kv_pieces)
    split = kv.reshape(block_count, BLK, 2, group_count, HEAD)

    def compress(which, w):
        flat = split[:, :, which].transpose(0, 2, 1, 3).reshape(-1, BLK * HEAD)
        out = jnp.dot(flat, w, preferred_element_type=jnp.float32).astype(jnp.bfloat16)
        return out.reshape(block_count, group_count * HEAD)

    comp = jnp.concatenate([compress(0, w_ckey), compress(1, w_cvalue)], axis=1)
    pad = -block_count % 16
    packed = jnp.concatenate([kv, jnp.pad(comp, ((0, pad), (0, 0)))], axis=0)
    if few:
        earlier = [
            lax.ppermute(packed, "kv", [(i, i + s) for i in range(spans - s)])
            for s in range(1, spans)
        ]
        every = jnp.stack([packed] + earlier)
        order = lax.rem(shard_index - jnp.arange(spans) + spans, spans)
        comp_all = every[:, tok_count : tok_count + block_count][order]
    else:
        every = lax.all_gather(packed, "kv", axis=0)
        comp_all = every[:, tok_count : tok_count + block_count]
    comp_all = comp_all.reshape(spans * block_count, -1)
    comp_all = jnp.pad(comp_all, ((0, -comp_all.shape[0] % LANES), (0, 0)))

    queries = project(w_query, query_pieces)

    attended = attend(
        (block_count, group_count, per_group, few),
        jnp.full((1,), shard_index, jnp.int32),
        block_picks[0].reshape(block_count, group_count * PICKS),
        queries,
        gates,
        every,
        comp_all,
    )

    if few:

        def finish(side):
            dims = (half_rows, width)
            at = place(side)
            return piece_product(out_kernel, spans, copies, at, attended, w_out, out_pieces, dims)

    else:
        out_parts = lax.all_gather(share(w_out), ("kv", "dp"), axis=0)
        out_parts = out_parts.reshape(spans, w_out.shape[0], w_out.shape[1])

        def finish(side):
            rows = lax.dynamic_slice_in_dim(attended, side * half_rows, half_rows, 0)
            parts = [
                jnp.dot(rows, out_parts[i], preferred_element_type=jnp.float32)
                for i in range(spans)
            ]
            return jnp.concatenate(parts, axis=1).astype(jnp.bfloat16)

    swap = [(i, 1 - i) for i in range(sides)]
    came = lax.ppermute(finish(1 - head_index), "tp", swap)
    mine = finish(head_index)
    summed = mine.astype(jnp.float32) + came.astype(jnp.float32)
    out_positions = (
        shard_index * tok_count + head_index * half_rows + jnp.arange(half_rows, dtype=jnp.int32)
    )
    live_rows = out_positions < seq_lengths[0]
    return jnp.where(live_rows[:, None], summed, 0.0).astype(jnp.bfloat16)[None]


def solution(mesh):
    return jax.shard_map(
        body,
        mesh=mesh,
        in_specs=(
            P("dp", "kv", None),
            P("dp"),
            P("dp", "kv", "tp", None),
            P("kv", "tp"),
            P("kv", "tp"),
            P("kv", "tp"),
            P(),
            P(),
            P(),
            P("tp", "kv"),
        ),
        out_specs=P("dp", ("kv", "tp"), None),
        check_vma=False,
    )
```

```python
import functools

import jax
import jax.numpy as jnp
from jax import lax
from jax.experimental import pallas as pl
from jax.experimental.pallas import tpu as pltpu
from jax.sharding import PartitionSpec as P

HEADS = 16
HEAD = 64
BLK = 64
PICKS = 16
LANES = 128

masked_low = -1e30


def nt_dot(a, b):
    return lax.dot_general(a, b, (((1,), (1,)), ((), ())), preferred_element_type=jnp.float32)


def group_slabs(slab, odd, low_lanes, high_lanes):
    rolled = jnp.concatenate([slab[:, HEAD:], slab[:, :HEAD]], axis=1)
    low, high = (rolled, slab) if odd else (slab, rolled)
    return jnp.concatenate([low * low_lanes, high * high_lanes], axis=0)


def attend_kernel(
    shape, start_ref, picks_ref, q_ref, gate_ref, pairs_ref, comp_ref, out_ref, spill_ref, list_ref
):
    blocks, groups, per_group, few, comp_step, spans = shape
    pairs = per_group // 2
    rows = pairs * BLK
    kv_width = groups * HEAD
    comp_count = comp_ref.shape[0]
    inv_scale = HEAD ** (-0.5)
    span = start_ref[0]
    lane_row = lax.broadcasted_iota(jnp.int32, (1, LANES), 1)
    low_lanes = jnp.where(lane_row < HEAD, 1.0, 0.0).astype(jnp.bfloat16)
    high_lanes = jnp.where(lane_row < HEAD, 0.0, 1.0).astype(jnp.bfloat16)
    lane = lax.broadcasted_iota(jnp.int32, (rows, LANES), 1)
    spot = lax.broadcasted_iota(jnp.int32, (rows, LANES), 0) % BLK
    low_half = lane < HEAD
    own_seen = low_half & (lane <= spot)
    high_half = jnp.logical_not(low_half)
    comp_lane = lax.broadcasted_iota(jnp.int32, (rows, comp_count), 1)
    comp_spot = lax.broadcasted_iota(jnp.int32, (rows, comp_count), 0) % BLK
    comp_at = comp_lane // comp_step
    comp_inner = comp_lane - comp_at * comp_step
    comp_span = span - comp_at if few else comp_at
    comp_real = (comp_inner < blocks) & (comp_at < spans) & (comp_span >= 0)
    comp_end = (comp_span * blocks + comp_inner + 1) * BLK - 1
    comp_end = jnp.where(comp_real, comp_end, jnp.iinfo(jnp.int32).max)

    def block_rows(block):
        at = block // blocks
        row = pl.multiple_of((block - at * blocks) * BLK, BLK)
        return span - at if few else at, pl.ds(row, BLK)

    def two_heads(s, n):
        return s[:, :n], s[:, n:]

    def top(s, mask):
        s = jnp.where(mask, s, masked_low)
        return s, jnp.max(s, axis=1, keepdims=True)

    def key_values(block_a, block_b, g):
        column = (g // 2) * LANES
        parts = []
        for base in (column, kv_width + column):
            a_span, a_rows = block_rows(block_a)
            b_span, b_rows = block_rows(block_b)
            slab = jnp.concatenate(
                [
                    pairs_ref[a_span, a_rows, base : base + LANES],
                    pairs_ref[b_span, b_rows, base : base + LANES],
                ],
                axis=0,
            )
            parts.append(group_slabs(slab, g % 2, low_lanes, high_lanes))
        return parts

    comp_parts = []
    for g in range(groups):
        column = (g // 2) * LANES
        comp_parts.append(
            [
                group_slabs(comp_ref[:, base : base + LANES], g % 2, low_lanes, high_lanes)
                for base in (column, kv_width + column)
            ]
        )

    def one_block(b, _):
        here = pl.ds(pl.multiple_of(b * BLK, BLK), BLK)
        gates = gate_ref[here, :]
        comp_seen = comp_end <= (span * blocks + b) * BLK + comp_spot
        counts, queries, comp_outs, scores, values_of = [], [], [], [], []
        for g in range(groups):
            count = jnp.int32(0)
            for k in range(PICKS):
                pick = picks_ref[b, g * PICKS + k]
                list_ref[g, count] = pick
                count = count + (pick >= 0).astype(jnp.int32)
            counts.append(count)
        for g in range(groups):
            slabs = [
                q_ref[here, (g * pairs + p) * LANES : (g * pairs + p + 1) * LANES]
                for p in range(pairs)
            ]
            queries.append(jnp.concatenate(slabs, axis=0))
            first = jnp.maximum(list_ref[g, 0], 0)
            keys, values = key_values(span * blocks + b, first, g)
            values_of.append(values)
            seen = own_seen | (high_half & (jnp.full((rows, LANES), counts[g]) > 0))
            for s in two_heads(nt_dot(queries[g], keys) * inv_scale, LANES):
                scores.append(top(s, seen))
        for g in range(groups):
            ckeys, cvalues = comp_parts[g]
            comp_probs = []
            for s in two_heads(nt_dot(queries[g], ckeys) * inv_scale, comp_count):
                s, m = top(s, comp_seen)
                w = jnp.where(comp_seen, jnp.exp(s - m), 0.0)
                total = jnp.maximum(jnp.sum(w, axis=1, keepdims=True), 1.0)
                comp_probs.append((w * (1.0 / total)).astype(jnp.bfloat16))
            comp_outs.append(
                jnp.dot(
                    jnp.concatenate(comp_probs, axis=1), cvalues, preferred_element_type=jnp.float32
                )
            )

        def far_blocks(g, i):
            second_there = 2 * i + 2 < counts[g]
            block_a = list_ref[g, 2 * i + 1]
            block_b = jnp.where(second_there, list_ref[g, 2 * i + 2], block_a)
            return block_a, block_b, second_there

        def scan(g, i, tops):
            block_a, block_b, second_there = far_blocks(g, i)
            far_keys, _ = key_values(block_a, block_b, g)
            limit = jnp.where(second_there, LANES, HEAD)
            far_seen = lane < jnp.full((rows, LANES), limit)
            s = two_heads(nt_dot(queries[g], far_keys) * inv_scale, LANES)
            (a, ma), (c, mc) = [top(x, far_seen) for x in s]
            spill_ref[g, i, :, :LANES] = a
            spill_ref[g, i, :, LANES:] = c
            return jnp.maximum(tops[0], ma), jnp.maximum(tops[1], mc)

        def add_up(g, i, sums):
            a = jnp.exp(spill_ref[g, i, :, :LANES] - tops[g][0])
            c = jnp.exp(spill_ref[g, i, :, LANES:] - tops[g][1])
            spill_ref[g, i, :, :LANES] = a
            spill_ref[g, i, :, LANES:] = c
            return (
                sums[0] + jnp.sum(a, axis=1, keepdims=True),
                sums[1] + jnp.sum(c, axis=1, keepdims=True),
            )

        def weigh(g, a, c, far_values):
            r0, r1 = scales[g]
            probs = jnp.concatenate(
                [(a * r0).astype(jnp.bfloat16), (c * r1).astype(jnp.bfloat16)], axis=1
            )
            return jnp.dot(probs, far_values, preferred_element_type=jnp.float32)

        def gather(g, i, total):
            block_a, block_b, _ = far_blocks(g, i)
            _, far_values = key_values(block_a, block_b, g)
            a, c = spill_ref[g, i, :, :LANES], spill_ref[g, i, :, LANES:]
            return total + weigh(g, a, c, far_values)

        steps = [count // 2 for count in counts]
        tops = [
            lax.fori_loop(
                0, steps[g], functools.partial(scan, g), (scores[2 * g][1], scores[2 * g + 1][1])
            )
            for g in range(groups)
        ]
        weights = [
            [jnp.exp(scores[2 * g + i][0] - tops[g][i]) for i in range(2)] for g in range(groups)
        ]
        sums = [tuple(jnp.sum(w, axis=1, keepdims=True) for w in weights[g]) for g in range(groups)]
        sums = [
            lax.fori_loop(0, steps[g], functools.partial(add_up, g), sums[g]) for g in range(groups)
        ]
        scales = [[1.0 / x for x in sums[g]] for g in range(groups)]
        outs = [weigh(g, weights[g][0], weights[g][1], values_of[g]) for g in range(groups)]
        outs = [
            lax.fori_loop(0, steps[g], functools.partial(gather, g), outs[g]) for g in range(groups)
        ]
        for g in range(groups):
            for p in range(pairs):
                h = g * per_group + 2 * p
                part = slice(p * BLK, (p + 1) * BLK)
                low = low_half[part]
                mix = []
                for branch in range(2):
                    at = branch * groups * per_group + h
                    mix.append(jnp.where(low, gates[:, at : at + 1], gates[:, at + 1 : at + 2]))
                mixed = mix[0] * comp_outs[g][part] + mix[1] * outs[g][part]
                column = (g * pairs + p) * LANES
                out_ref[here, column : column + LANES] = mixed.astype(jnp.bfloat16)
        return 0

    lax.fori_loop(0, blocks, one_block, 0)


def attend(shape, span, picks, queries, gates, pairs, comp):
    _, groups, per_group, _, _, _ = shape
    rows = per_group // 2 * BLK
    smem = pl.BlockSpec(memory_space=pltpu.SMEM)
    vmem = pl.BlockSpec(memory_space=pltpu.VMEM)
    return pl.pallas_call(
        functools.partial(attend_kernel, shape),
        out_shape=jax.ShapeDtypeStruct(queries.shape, jnp.bfloat16),
        in_specs=[smem, smem, vmem, vmem, vmem, vmem],
        out_specs=vmem,
        scratch_shapes=[
            pltpu.VMEM((groups, PICKS // 2, rows, 2 * LANES), jnp.float32),
            pltpu.SMEM((groups, PICKS + 2), jnp.int32),
        ],
        cost_estimate=pl.CostEstimate(
            flops=int(1e10), bytes_accessed=int(4e6), transcendentals=int(1e6)
        ),
    )(span, picks, queries, gates, pairs, comp)


def along_kv(w, spans):
    return [
        lax.ppermute(w, "kv", [(i, (i + s) % spans) for i in range(spans)])
        for s in range(1, spans)
    ]


def along_dp(came, copies):
    stack = jnp.concatenate(came, axis=0)
    return [stack] + [
        lax.ppermute(stack, "dp", [(i, i ^ m) for i in range(copies)]) for m in range(1, copies)
    ]


def piece_places(spans, copies, me, copy):
    return [
        (m, s - 1, lax.rem(me - s + spans, spans), copy ^ m)
        for s in range(1, spans)
        for m in range(copies)
    ]


def project_kernel(spans, copies, at_ref, x_ref, own_ref, *refs):
    *pieces, out_ref = refs
    rows = own_ref.shape[0]
    part = rows // copies
    me, copy = at_ref[0], at_ref[1]
    total = jnp.dot(
        x_ref[:, pl.ds(pl.multiple_of(me * rows, LANES), rows)],
        own_ref[...],
        preferred_element_type=jnp.float32,
    )
    for m, at, span, owner in piece_places(spans, copies, me, copy):
        start = pl.multiple_of(span * rows + owner * part, LANES)
        total = total + jnp.dot(
            x_ref[:, pl.ds(start, part)],
            pieces[m][at * part : (at + 1) * part, :],
            preferred_element_type=jnp.float32,
        )
    out_ref[...] = total.astype(out_ref.dtype)


def out_kernel(spans, copies, at_ref, x_ref, own_ref, *refs):
    *pieces, out_ref = refs
    depth, width = own_ref.shape
    part = depth // copies
    me, copy, side = at_ref[0], at_ref[1], at_ref[2]
    count = out_ref.shape[0]
    rows = pl.ds(pl.multiple_of(side * count, 16), count)
    start = pl.multiple_of(me * width, LANES)
    out_ref[:, pl.ds(start, width)] = jnp.dot(
        x_ref[rows, :], own_ref[...], preferred_element_type=jnp.float32
    ).astype(out_ref.dtype)
    places = piece_places(spans, copies, me, copy)
    for s in range(spans - 1):
        total = None
        for m, at, span, owner in places[s * copies : (s + 1) * copies]:
            term = jnp.dot(
                x_ref[rows, pl.ds(pl.multiple_of(owner * part, LANES), part)],
                pieces[m][at * part : (at + 1) * part, :],
                preferred_element_type=jnp.float32,
            )
            total = term if total is None else total + term
        start = pl.multiple_of(span * width, LANES)
        out_ref[:, pl.ds(start, width)] = total.astype(out_ref.dtype)


def piece_product(kernel, spans, copies, at, x, own, pieces, out_dims):
    vmem = pl.BlockSpec(memory_space=pltpu.VMEM)
    return pl.pallas_call(
        functools.partial(kernel, spans, copies),
        out_shape=jax.ShapeDtypeStruct(out_dims, jnp.bfloat16),
        in_specs=[pl.BlockSpec(memory_space=pltpu.SMEM)] + [vmem] * (2 + len(pieces)),
        out_specs=vmem,
        cost_estimate=pl.CostEstimate(
            flops=2 * out_dims[0] * out_dims[1] * x.shape[1],
            bytes_accessed=int(4e6),
            transcendentals=0,
        ),
    )(at, x, own, *pieces)


def body(
    tokens, seq_lengths, block_picks, w_query, w_key, w_value, w_gate, w_ckey, w_cvalue, w_out
):
    token_rows = tokens[0]
    tok_count = token_rows.shape[0]
    width = token_rows.shape[1]
    spans = lax.axis_size("kv")
    copies = lax.axis_size("dp")
    sides = lax.axis_size("tp")
    shard_index = lax.axis_index("kv")
    head_index = lax.axis_index("tp")
    copy_index = lax.axis_index("dp")
    group_count = w_key.shape[1] // HEAD
    head_count = w_query.shape[1] // HEAD
    per_group = head_count // group_count
    block_count = tok_count // BLK
    half_rows = tok_count // sides
    w_both = jnp.concatenate([w_key, w_value], axis=1)
    few = spans <= 8 and copies & (copies - 1) == 0
    few = few and w_both.shape[0] % (copies * LANES) == 0 and w_out.shape[0] % (copies * LANES) == 0
    few = few and w_query.shape[1] == w_out.shape[1]

    def place(side):
        return jnp.stack([shard_index, copy_index, side]).astype(jnp.int32)

    def share(w):
        part = w.shape[0] // copies
        return lax.dynamic_slice_in_dim(w, copy_index * part, part, 0)

    def project(w, pieces):
        if few:
            dims = (tok_count, w.shape[1])
            at = place(head_index)
            return piece_product(project_kernel, spans, copies, at, token_rows, w, pieces, dims)
        whole = lax.all_gather(share(w), ("kv", "dp"), axis=0, tiled=True)
        out = jnp.dot(token_rows, whole, preferred_element_type=jnp.float32)
        return out.astype(jnp.bfloat16)

    kv_pieces = query_pieces = out_pieces = None
    if few:
        kv_pieces = along_dp(along_kv(share(w_both), spans), copies)
        part = w_query.shape[0] // copies
        came = along_kv(jnp.concatenate([share(w_query), share(w_out)], axis=0), spans)
        query_pieces = along_dp([c[:part] for c in came], copies)
        out_pieces = along_dp([c[part:] for c in came], copies)

    gate_all = jax.nn.sigmoid(jnp.dot(token_rows, w_gate, preferred_element_type=jnp.float32))
    gates = lax.dynamic_slice_in_dim(
        gate_all.reshape(tok_count, 2, HEADS), head_index * head_count, head_count, 2
    ).reshape(tok_count, 2 * head_count)

    kv = project(w_both, kv_pieces)
    split = kv.reshape(block_count, BLK, 2, group_count, HEAD)

    def compress(which, w):
        flat = split[:, :, which].transpose(0, 2, 1, 3).reshape(-1, BLK * HEAD)
        out = jnp.dot(flat, w, preferred_element_type=jnp.float32).astype(jnp.bfloat16)
        return out.reshape(block_count, group_count * HEAD)

    comp = jnp.concatenate([compress(0, w_ckey), compress(1, w_cvalue)], axis=1)
    pad = -block_count % 16
    packed = jnp.concatenate([kv, jnp.pad(comp, ((0, pad), (0, 0)))], axis=0)
    if few:
        earlier = [
            lax.ppermute(packed, "kv", [(i, i + s) for i in range(spans - s)])
            for s in range(1, spans)
        ]
        every = jnp.stack([packed] + earlier)
    else:
        every = lax.all_gather(packed, "kv", axis=0)
    comp_all = every[:, tok_count:].reshape(spans * (block_count + pad), -1)
    comp_all = jnp.pad(comp_all, ((0, -comp_all.shape[0] % LANES), (0, 0)))

    queries = project(w_query, query_pieces)

    attended = attend(
        (block_count, group_count, per_group, few, block_count + pad, spans),
        jnp.full((1,), shard_index, jnp.int32),
        block_picks[0].reshape(block_count, group_count * PICKS),
        queries,
        gates,
        every,
        comp_all,
    )

    if few:

        def finish(side):
            dims = (half_rows, width)
            at = place(side)
            return piece_product(out_kernel, spans, copies, at, attended, w_out, out_pieces, dims)

    else:
        out_parts = lax.all_gather(share(w_out), ("kv", "dp"), axis=0)
        out_parts = out_parts.reshape(spans, w_out.shape[0], w_out.shape[1])

        def finish(side):
            rows = lax.dynamic_slice_in_dim(attended, side * half_rows, half_rows, 0)
            parts = [
                jnp.dot(rows, out_parts[i], preferred_element_type=jnp.float32)
                for i in range(spans)
            ]
            return jnp.concatenate(parts, axis=1).astype(jnp.bfloat16)

    swap = [(i, 1 - i) for i in range(sides)]
    came = lax.ppermute(finish(1 - head_index), "tp", swap)
    mine = finish(head_index)
    summed = mine.astype(jnp.float32) + came.astype(jnp.float32)
    out_positions = (
        shard_index * tok_count + head_index * half_rows + jnp.arange(half_rows, dtype=jnp.int32)
    )
    live_rows = out_positions < seq_lengths[0]
    return jnp.where(live_rows[:, None], summed, 0.0).astype(jnp.bfloat16)[None]


def solution(mesh):
    return jax.shard_map(
        body,
        mesh=mesh,
        in_specs=(
            P("dp", "kv", None),
            P("dp"),
            P("dp", "kv", "tp", None),
            P("kv", "tp"),
            P("kv", "tp"),
            P("kv", "tp"),
            P(),
            P(),
            P(),
            P("tp", "kv"),
        ),
        out_specs=P("dp", ("kv", "tp"), None),
        check_vma=False,
    )
```

```python
import functools

import jax
import jax.numpy as jnp
from jax import lax
from jax.experimental import pallas as pl
from jax.experimental.pallas import tpu as pltpu
from jax.sharding import PartitionSpec as P

HEADS = 16
HEAD = 64
BLK = 64
PICKS = 16
LANES = 128

masked_low = -1e30


def nt_dot(a, b):
    return lax.dot_general(a, b, (((1,), (1,)), ((), ())), preferred_element_type=jnp.float32)


def group_slabs(slab, odd, low_lanes, high_lanes):
    rolled = jnp.concatenate([slab[:, HEAD:], slab[:, :HEAD]], axis=1)
    low, high = (rolled, slab) if odd else (slab, rolled)
    return jnp.concatenate([low * low_lanes, high * high_lanes], axis=0)


def attend_kernel(
    shape, start_ref, picks_ref, q_ref, gate_ref, pairs_ref, comp_ref, out_ref, spill_ref, list_ref
):
    blocks, groups, per_group, few, comp_step, spans = shape
    pairs = per_group // 2
    rows = pairs * BLK
    kv_width = groups * HEAD
    comp_count = comp_ref.shape[0]
    inv_scale = HEAD ** (-0.5)
    span = start_ref[0]
    lane_row = lax.broadcasted_iota(jnp.int32, (1, LANES), 1)
    low_lanes = jnp.where(lane_row < HEAD, 1.0, 0.0).astype(jnp.bfloat16)
    high_lanes = jnp.where(lane_row < HEAD, 0.0, 1.0).astype(jnp.bfloat16)
    lane = lax.broadcasted_iota(jnp.int32, (rows, LANES), 1)
    spot = lax.broadcasted_iota(jnp.int32, (rows, LANES), 0) % BLK
    low_half = lane < HEAD
    own_seen = low_half & (lane <= spot)
    high_half = jnp.logical_not(low_half)
    comp_lane = lax.broadcasted_iota(jnp.int32, (rows, comp_count), 1)
    comp_spot = lax.broadcasted_iota(jnp.int32, (rows, comp_count), 0) % BLK
    comp_at = comp_lane // comp_step
    comp_inner = comp_lane - comp_at * comp_step
    comp_span = span - comp_at if few else comp_at
    comp_real = (comp_inner < blocks) & (comp_at < spans) & (comp_span >= 0)
    comp_end = (comp_span * blocks + comp_inner + 1) * BLK - 1
    comp_end = jnp.where(comp_real, comp_end, jnp.iinfo(jnp.int32).max)

    def block_rows(block):
        at = block // blocks
        row = pl.multiple_of((block - at * blocks) * BLK, BLK)
        return span - at if few else at, pl.ds(row, BLK)

    def two_heads(s, n):
        return s[:, :n], s[:, n:]

    def top(s, mask):
        s = jnp.where(mask, s, masked_low)
        return s, jnp.max(s, axis=1, keepdims=True)

    def key_values(block_a, block_b, g):
        column = (g // 2) * LANES
        parts = []
        for base in (column, kv_width + column):
            a_span, a_rows = block_rows(block_a)
            b_span, b_rows = block_rows(block_b)
            slab = jnp.concatenate(
                [
                    pairs_ref[a_span, a_rows, base : base + LANES],
                    pairs_ref[b_span, b_rows, base : base + LANES],
                ],
                axis=0,
            )
            parts.append(group_slabs(slab, g % 2, low_lanes, high_lanes))
        return parts

    comp_parts = []
    for g in range(groups):
        column = (g // 2) * LANES
        comp_parts.append(
            [
                group_slabs(comp_ref[:, base : base + LANES], g % 2, low_lanes, high_lanes)
                for base in (column, kv_width + column)
            ]
        )

    def one_block(b, _):
        here = pl.ds(pl.multiple_of(b * BLK, BLK), BLK)
        gates = gate_ref[here, :]
        comp_seen = comp_end <= (span * blocks + b) * BLK + comp_spot
        counts, queries, comp_outs, scores, values_of = [], [], [], [], []
        for g in range(groups):
            count = jnp.int32(0)
            for k in range(PICKS):
                pick = picks_ref[b, g * PICKS + k]
                list_ref[g, count] = pick
                count = count + (pick >= 0).astype(jnp.int32)
            counts.append(count)
        for g in range(groups):
            slabs = [
                q_ref[here, (g * pairs + p) * LANES : (g * pairs + p + 1) * LANES]
                for p in range(pairs)
            ]
            queries.append(jnp.concatenate(slabs, axis=0))
            first = jnp.maximum(list_ref[g, 0], 0)
            keys, values = key_values(span * blocks + b, first, g)
            values_of.append(values)
            seen = own_seen | (high_half & (jnp.full((rows, LANES), counts[g]) > 0))
            for s in two_heads(nt_dot(queries[g], keys) * inv_scale, LANES):
                scores.append(top(s, seen))
        for g in range(groups):
            ckeys, cvalues = comp_parts[g]
            comp_probs = []
            for s in two_heads(nt_dot(queries[g], ckeys) * inv_scale, comp_count):
                s, m = top(s, comp_seen)
                w = jnp.where(comp_seen, jnp.exp(s - m), 0.0)
                total = jnp.maximum(jnp.sum(w, axis=1, keepdims=True), 1.0)
                comp_probs.append((w * (1.0 / total)).astype(jnp.bfloat16))
            comp_outs.append(
                jnp.dot(
                    jnp.concatenate(comp_probs, axis=1), cvalues, preferred_element_type=jnp.float32
                )
            )

        def far_blocks(g, i):
            second_there = 2 * i + 2 < counts[g]
            block_a = list_ref[g, 2 * i + 1]
            block_b = jnp.where(second_there, list_ref[g, 2 * i + 2], block_a)
            return block_a, block_b, second_there

        def scan(g, i, tops):
            block_a, block_b, second_there = far_blocks(g, i)
            far_keys, _ = key_values(block_a, block_b, g)
            limit = jnp.where(second_there, LANES, HEAD)
            far_seen = lane < jnp.full((rows, LANES), limit)
            s = two_heads(nt_dot(queries[g], far_keys) * inv_scale, LANES)
            (a, ma), (c, mc) = [top(x, far_seen) for x in s]
            spill_ref[g, i, :, :LANES] = a
            spill_ref[g, i, :, LANES:] = c
            return jnp.maximum(tops[0], ma), jnp.maximum(tops[1], mc)

        def add_up(g, i, sums):
            a = jnp.exp(spill_ref[g, i, :, :LANES] - tops[g][0])
            c = jnp.exp(spill_ref[g, i, :, LANES:] - tops[g][1])
            spill_ref[g, i, :, :LANES] = a
            spill_ref[g, i, :, LANES:] = c
            return (
                sums[0] + jnp.sum(a, axis=1, keepdims=True),
                sums[1] + jnp.sum(c, axis=1, keepdims=True),
            )

        def weigh(g, a, c, far_values):
            r0, r1 = scales[g]
            probs = jnp.concatenate(
                [(a * r0).astype(jnp.bfloat16), (c * r1).astype(jnp.bfloat16)], axis=1
            )
            return jnp.dot(probs, far_values, preferred_element_type=jnp.float32)

        def gather(g, i, total):
            block_a, block_b, _ = far_blocks(g, i)
            _, far_values = key_values(block_a, block_b, g)
            a, c = spill_ref[g, i, :, :LANES], spill_ref[g, i, :, LANES:]
            return total + weigh(g, a, c, far_values)

        steps = [count // 2 for count in counts]
        tops = [
            lax.fori_loop(
                0, steps[g], functools.partial(scan, g), (scores[2 * g][1], scores[2 * g + 1][1])
            )
            for g in range(groups)
        ]
        weights = [
            [jnp.exp(scores[2 * g + i][0] - tops[g][i]) for i in range(2)] for g in range(groups)
        ]
        sums = [tuple(jnp.sum(w, axis=1, keepdims=True) for w in weights[g]) for g in range(groups)]
        sums = [
            lax.fori_loop(0, steps[g], functools.partial(add_up, g), sums[g]) for g in range(groups)
        ]
        scales = [[1.0 / x for x in sums[g]] for g in range(groups)]
        outs = [weigh(g, weights[g][0], weights[g][1], values_of[g]) for g in range(groups)]
        outs = [
            lax.fori_loop(0, steps[g], functools.partial(gather, g), outs[g]) for g in range(groups)
        ]
        for g in range(groups):
            for p in range(pairs):
                h = g * per_group + 2 * p
                part = slice(p * BLK, (p + 1) * BLK)
                low = low_half[part]
                mix = []
                for branch in range(2):
                    at = branch * groups * per_group + h
                    mix.append(jnp.where(low, gates[:, at : at + 1], gates[:, at + 1 : at + 2]))
                mixed = mix[0] * comp_outs[g][part] + mix[1] * outs[g][part]
                column = (g * pairs + p) * LANES
                out_ref[here, column : column + LANES] = mixed.astype(jnp.bfloat16)
        return 0

    lax.fori_loop(0, blocks, one_block, 0)


def attend(shape, span, picks, queries, gates, pairs, comp):
    _, groups, per_group, _, _, _ = shape
    rows = per_group // 2 * BLK
    smem = pl.BlockSpec(memory_space=pltpu.SMEM)
    vmem = pl.BlockSpec(memory_space=pltpu.VMEM)
    return pl.pallas_call(
        functools.partial(attend_kernel, shape),
        out_shape=jax.ShapeDtypeStruct(queries.shape, jnp.bfloat16),
        in_specs=[smem, smem, vmem, vmem, vmem, vmem],
        out_specs=vmem,
        scratch_shapes=[
            pltpu.VMEM((groups, PICKS // 2, rows, 2 * LANES), jnp.float32),
            pltpu.SMEM((groups, PICKS + 2), jnp.int32),
        ],
        cost_estimate=pl.CostEstimate(
            flops=int(1e10), bytes_accessed=int(4e6), transcendentals=int(1e6)
        ),
    )(span, picks, queries, gates, pairs, comp)


def along_kv(w, spans):
    return [
        lax.ppermute(w, "kv", [(i, (i + s) % spans) for i in range(spans)])
        for s in range(1, spans)
    ]


def along_dp(came, copies):
    stack = jnp.concatenate(came, axis=0)
    return [stack] + [
        lax.ppermute(stack, "dp", [(i, i ^ m) for i in range(copies)]) for m in range(1, copies)
    ]


def piece_places(spans, copies, me, copy):
    return [
        (m, s - 1, lax.rem(me - s + spans, spans), copy ^ m)
        for s in range(1, spans)
        for m in range(copies)
    ]


def project_kernel(spans, copies, at_ref, x_ref, own_ref, *refs):
    *pieces, out_ref = refs
    rows = own_ref.shape[0]
    part = rows // copies
    me, copy = at_ref[0], at_ref[1]
    total = jnp.dot(
        x_ref[:, pl.ds(pl.multiple_of(me * rows, LANES), rows)],
        own_ref[...],
        preferred_element_type=jnp.float32,
    )
    for m, at, span, owner in piece_places(spans, copies, me, copy):
        start = pl.multiple_of(span * rows + owner * part, LANES)
        total = total + jnp.dot(
            x_ref[:, pl.ds(start, part)],
            pieces[m][at * part : (at + 1) * part, :],
            preferred_element_type=jnp.float32,
        )
    out_ref[...] = total.astype(out_ref.dtype)


def out_kernel(spans, copies, at_ref, x_ref, own_ref, *refs):
    *pieces, out_ref = refs
    depth, width = own_ref.shape
    part = depth // copies
    me, copy, side = at_ref[0], at_ref[1], at_ref[2]
    count = out_ref.shape[0]
    rows = pl.ds(pl.multiple_of(side * count, 16), count)
    start = pl.multiple_of(me * width, LANES)
    out_ref[:, pl.ds(start, width)] = jnp.dot(
        x_ref[rows, :], own_ref[...], preferred_element_type=jnp.float32
    ).astype(out_ref.dtype)
    places = piece_places(spans, copies, me, copy)
    for s in range(spans - 1):
        total = None
        for m, at, span, owner in places[s * copies : (s + 1) * copies]:
            term = jnp.dot(
                x_ref[rows, pl.ds(pl.multiple_of(owner * part, LANES), part)],
                pieces[m][at * part : (at + 1) * part, :],
                preferred_element_type=jnp.float32,
            )
            total = term if total is None else total + term
        start = pl.multiple_of(span * width, LANES)
        out_ref[:, pl.ds(start, width)] = total.astype(out_ref.dtype)


def piece_product(kernel, spans, copies, at, x, own, pieces, out_dims):
    vmem = pl.BlockSpec(memory_space=pltpu.VMEM)
    return pl.pallas_call(
        functools.partial(kernel, spans, copies),
        out_shape=jax.ShapeDtypeStruct(out_dims, jnp.bfloat16),
        in_specs=[pl.BlockSpec(memory_space=pltpu.SMEM)] + [vmem] * (2 + len(pieces)),
        out_specs=vmem,
        cost_estimate=pl.CostEstimate(
            flops=2 * out_dims[0] * out_dims[1] * x.shape[1],
            bytes_accessed=int(4e6),
            transcendentals=0,
        ),
    )(at, x, own, *pieces)


def body(
    tokens, seq_lengths, block_picks, w_query, w_key, w_value, w_gate, w_ckey, w_cvalue, w_out
):
    token_rows = tokens[0]
    tok_count = token_rows.shape[0]
    width = token_rows.shape[1]
    spans = lax.axis_size("kv")
    copies = lax.axis_size("dp")
    sides = lax.axis_size("tp")
    shard_index = lax.axis_index("kv")
    head_index = lax.axis_index("tp")
    copy_index = lax.axis_index("dp")
    group_count = w_key.shape[1] // HEAD
    head_count = w_query.shape[1] // HEAD
    per_group = head_count // group_count
    block_count = tok_count // BLK
    half_rows = tok_count // sides
    w_both = jnp.concatenate([w_key, w_value], axis=1)
    few = spans <= 8 and copies & (copies - 1) == 0
    few = few and w_both.shape[0] % (copies * LANES) == 0 and w_out.shape[0] % (copies * LANES) == 0
    few = few and w_query.shape[1] == w_out.shape[1]

    def place(side):
        return jnp.stack([shard_index, copy_index, side]).astype(jnp.int32)

    def share(w):
        part = w.shape[0] // copies
        return lax.dynamic_slice_in_dim(w, copy_index * part, part, 0)

    def project(w, pieces):
        if few:
            dims = (tok_count, w.shape[1])
            at = place(head_index)
            return piece_product(project_kernel, spans, copies, at, token_rows, w, pieces, dims)
        whole = lax.all_gather(share(w), ("kv", "dp"), axis=0, tiled=True)
        out = jnp.dot(token_rows, whole, preferred_element_type=jnp.float32)
        return out.astype(jnp.bfloat16)

    kv_pieces = query_pieces = out_pieces = None
    if few:
        kv_pieces = along_dp(along_kv(share(w_both), spans), copies)
        part = w_query.shape[0] // copies
        came = along_kv(jnp.concatenate([share(w_query), share(w_out)], axis=0), spans)

    gate_all = jax.nn.sigmoid(jnp.dot(token_rows, w_gate, preferred_element_type=jnp.float32))
    gates = lax.dynamic_slice_in_dim(
        gate_all.reshape(tok_count, 2, HEADS), head_index * head_count, head_count, 2
    ).reshape(tok_count, 2 * head_count)

    kv = project(w_both, kv_pieces)
    split = kv.reshape(block_count, BLK, 2, group_count, HEAD)

    def compress(which, w):
        flat = split[:, :, which].transpose(0, 2, 1, 3).reshape(-1, BLK * HEAD)
        out = jnp.dot(flat, w, preferred_element_type=jnp.float32).astype(jnp.bfloat16)
        return out.reshape(block_count, group_count * HEAD)

    comp = jnp.concatenate([compress(0, w_ckey), compress(1, w_cvalue)], axis=1)
    pad = -block_count % 16
    packed = jnp.concatenate([kv, jnp.pad(comp, ((0, pad), (0, 0)))], axis=0)
    if few:
        came, _ = lax.optimization_barrier((came, packed))
        query_pieces = along_dp([c[:part] for c in came], copies)
        out_pieces = along_dp([c[part:] for c in came], copies)
        earlier = [
            lax.ppermute(packed, "kv", [(i, i + s) for i in range(spans - s)])
            for s in range(1, spans)
        ]
        every = jnp.stack([packed] + earlier)
    else:
        every = lax.all_gather(packed, "kv", axis=0)
    comp_all = every[:, tok_count:].reshape(spans * (block_count + pad), -1)
    comp_all = jnp.pad(comp_all, ((0, -comp_all.shape[0] % LANES), (0, 0)))

    queries = project(w_query, query_pieces)

    attended = attend(
        (block_count, group_count, per_group, few, block_count + pad, spans),
        jnp.full((1,), shard_index, jnp.int32),
        block_picks[0].reshape(block_count, group_count * PICKS),
        queries,
        gates,
        every,
        comp_all,
    )

    if few:

        def finish(side):
            dims = (half_rows, width)
            at = place(side)
            return piece_product(out_kernel, spans, copies, at, attended, w_out, out_pieces, dims)

    else:
        out_parts = lax.all_gather(share(w_out), ("kv", "dp"), axis=0)
        out_parts = out_parts.reshape(spans, w_out.shape[0], w_out.shape[1])

        def finish(side):
            rows = lax.dynamic_slice_in_dim(attended, side * half_rows, half_rows, 0)
            parts = [
                jnp.dot(rows, out_parts[i], preferred_element_type=jnp.float32)
                for i in range(spans)
            ]
            return jnp.concatenate(parts, axis=1).astype(jnp.bfloat16)

    swap = [(i, 1 - i) for i in range(sides)]
    came = lax.ppermute(finish(1 - head_index), "tp", swap)
    mine = finish(head_index)
    summed = mine.astype(jnp.float32) + came.astype(jnp.float32)
    out_positions = (
        shard_index * tok_count + head_index * half_rows + jnp.arange(half_rows, dtype=jnp.int32)
    )
    live_rows = out_positions < seq_lengths[0]
    return jnp.where(live_rows[:, None], summed, 0.0).astype(jnp.bfloat16)[None]


def solution(mesh):
    return jax.shard_map(
        body,
        mesh=mesh,
        in_specs=(
            P("dp", "kv", None),
            P("dp"),
            P("dp", "kv", "tp", None),
            P("kv", "tp"),
            P("kv", "tp"),
            P("kv", "tp"),
            P(),
            P(),
            P(),
            P("tp", "kv"),
        ),
        out_specs=P("dp", ("kv", "tp"), None),
        check_vma=False,
    )
```
